32 devices in a mesh: grp: 2 (over y), ep: 16 (over z, x, core), tp: 1.
Axes of the slice: x: 2, y: 2, z: 4, core: 2. Of those that a mesh axis runs over, the one named last changes fastest.
Arguments:
- tokens: bfloat16 [2048, 2048], P(('grp', 'ep')), parts along dimension 0, may hold values from -6 to 6
- norm_gain: float32 [2048], replicated, may hold values from 0.1 to 1.9
- routes: int32 [2048, 6], P(('grp', 'ep')), parts along dimension 0, may hold values from 0 to 15, all different within a row; in each aligned block of 64 rows (0 to 63, 64 to 127, ...) at most 48 rows name the same one
- route_weights: float32 [2048, 6], P(('grp', 'ep')), parts along dimension 0, may hold values from 0.05 to 1
- w_gate: bfloat16 [16, 2048, 2048], P('ep', None, 'tp'), may hold values from -0.125 to 0.125
- w_up: bfloat16 [16, 2048, 2048], P('ep', None, 'tp'), may hold values from -0.125 to 0.125
- w_down: bfloat16 [16, 2048, 2048], P('ep', 'tp'), may hold values from -4 to 4
- final_gain: float32 [2048], P('tp'), may hold values from 0.1 to 1.9
Outputs:
- mixed_out: bfloat16 [2048, 2048], P(('grp', 'ep'), 'tp'), parts along dimension 0
The draws below stay inside these ranges and needn't reach their ends.
There are 2 independent parts, one for each index of `grp`. The reference program is written for one: setup_inputs(seed, part) draws one part's arguments, and reference() takes and returns one part's arrays. A program takes and returns all parts, laid end to end along the dimension named above; an argument that names none is the same for every part. Nothing has to cross between parts.
Inputs may be any that keep to these rules, and one draw needn't show every extreme that they name: `routes`: each row names 6 different experts; within the rows of one index of ep no expert is named by more than 48 rows, and in every draw some expert is named by exactly 48 rows of some index.
All inputs are finite; a program needn't handle non-finite values.
Results may differ from the reference program's by a relative error of at most 0.015.
Values may be sent and summed in bfloat16 or wider, within the bound.
A program may use at most 64 MiB of HBM per device.

```python
import math
import jax
import jax.numpy as jnp
import numpy as np
from jax import lax

D = 2048
FF = 2048
TOP_K = 6
TOK_DEV = 64
EXPERTS = 16
CAP = 48
TOKENS = 1024
N_EP = 16
N_TP = 1


def draw_w_down(key, part):
    key_values, key_columns = jax.random.split(key)
    columns = jnp.arange(D, dtype=jnp.float32) / D
    roughness = jax.random.uniform(key_columns, (D,), jnp.float32, 0.5, 1.5)
    values = jnp.clip(jax.random.normal(key_values, (EXPERTS, FF, D), jnp.float32), -5.0, 5.0)
    column_scale = jnp.exp(columns * jnp.log(10.0)) * roughness
    scaled = values * column_scale[None, None, :] * FF ** (-0.5) / 3.0
    return scaled.astype(jnp.bfloat16)


def block_scale(own_key, shape, cuts, smallest, high):
    loudness, own = 1.0, jax.random.fold_in(own_key, 6)
    for position, blocks in cuts:
        steps = jnp.exp(jax.random.uniform(jax.random.fold_in(own, position), (blocks,), jnp.float32, smallest / len(cuts), high / len(cuts)))
        loudness = loudness * jnp.repeat(steps, shape[position] // blocks).reshape([-1 if axis == position else 1 for axis in range(len(shape))])
    return loudness


def deal_out(key, own, number, rows, count, top, reach, slope):
    order = jax.random.permutation(key, count)
    crowded, common = load_shares(count, rows * top, reach, slope, True), load_shares(count, rows * top, reach, slope, False)
    places = jnp.arange(count)

    def named(sizes, offset_by):
        used = int((sizes > 0).sum())
        fixed = max(1, used // 4)
        shifted = fixed + (places - fixed + offset_by * (used - fixed)) % max(1, count - fixed)
        return jnp.zeros((count,), jnp.int32).at[order[jnp.where(places < fixed, places, shifted)]].set(jnp.asarray(sizes, jnp.int32))

    sizes = jnp.where(number % 4 == 0, named(crowded, number // 4), named(common, number - number // 4 - 1))
    mixed = jax.random.permutation(jax.random.fold_in(own, 3), count)
    source_of, taker = mixed[0:count // 2 * 2:2], mixed[1:count // 2 * 2:2]
    margin = jnp.minimum(sizes[source_of] - 1, reach - sizes[taker]) // 2
    margin = jnp.where((source_of == order[0]) | (taker == order[0]) | (sizes[taker] == 0), 0, jnp.maximum(margin, 0))
    shifted = jax.random.randint(jax.random.fold_in(own, 4), (count // 2,), 0, 1 << 20) % (margin + 1)
    sizes = sizes.at[source_of].add(-shifted).at[taker].add(shifted)
    labels = jnp.searchsorted(jnp.cumsum(sizes), jnp.arange(rows * top), side="right").astype(jnp.int32)
    listing = labels.reshape(top, rows).T
    listing = listing[jax.random.permutation(jax.random.fold_in(own, 1), rows)]
    offset_by = jax.random.randint(jax.random.fold_in(own, 2), (rows, 1), 0, top)
    return jnp.take_along_axis(listing, (jnp.arange(top)[None, :] + offset_by) % top, axis=1)


def load_shares(number_of, total, reach, slope, full):
    weights = [(1 << 20) // math.isqrt(standing ** slope) + 1 for standing in range(1, number_of + 1)]
    largest = reach if full else min(reach, max(-(-total // number_of), total * weights[0] // sum(weights)))
    least = 1 if total - largest >= number_of - 1 else 0
    counts, surplus = [largest] + [least] * (number_of - 1), total - largest - least * (number_of - 1)
    while surplus > 0:
        candidates = [i for i in range(1, number_of) if counts[i] < largest] or [i for i in range(1, number_of) if counts[i] < reach]
        mass, left = sum([weights[i] for i in candidates]), surplus
        for i in candidates:
            more = min(reach - counts[i], max(1, left * weights[i] // mass), surplus)
            counts[i] = counts[i] + more
            surplus = surplus - more
    return np.array(counts)


def scatter_about(rng, shape, deviation, bound, cuts=(), kind=jnp.bfloat16):
    loudness = block_scale(rng, shape, cuts, -0.22, 0.18) if cuts else 1.0
    array = jax.random.normal(rng, shape, jnp.float32) * deviation * loudness
    return jnp.minimum(jnp.maximum(array, -bound), bound).astype(kind)


def setup_inputs(seed: int = 0, part: int = 0) -> dict:
    keys = jax.random.split(jax.random.key(seed), 9)
    part_splits = jax.random.split(jax.random.fold_in(keys[8], part), 9)
    tokens = scatter_about(part_splits[0], (TOKENS, D), 1.0, 6.0, ((0, 16),))
    norm_gain = jnp.clip(1.0 + 0.18 * jax.random.normal(keys[1], (D,), jnp.float32), 0.1, 1.9)
    routes_keys = jax.random.split(jax.random.fold_in(part_splits[2], 1), TOKENS // TOK_DEV)
    routes_turns = jax.random.permutation(jax.random.fold_in(part_splits[2], 3), TOKENS // TOK_DEV)
    routes = jax.vmap(lambda own, number: deal_out(jax.random.fold_in(part_splits[2], 2), own, number, TOK_DEV, EXPERTS, TOP_K, CAP, 2))(routes_keys, routes_turns).reshape((TOKENS, TOP_K))
    route_weights = jnp.clip(jnp.exp(math.log(1.0) - 2.9957323 * jax.random.uniform(part_splits[3], (TOKENS, TOP_K), jnp.float32) ** block_scale(part_splits[3], (TOKENS, TOP_K), ((0, 16),), -0.2, 0.2)), 0.05, 1.0)
    w_gate = scatter_about(keys[4], (EXPERTS, D, FF), D ** -0.5, 0.125, ((0, 16),))
    w_up = scatter_about(keys[5], (EXPERTS, D, FF), D ** -0.5, 0.125, ((0, 16),))
    w_down = draw_w_down(jax.random.fold_in(keys[8], 71), part)
    final_gain = jnp.clip(1.0 + 0.18 * jax.random.normal(keys[7], (D,), jnp.float32), 0.1, 1.9)
    return dict(tokens=tokens, norm_gain=norm_gain, routes=routes, route_weights=route_weights, w_gate=w_gate, w_up=w_up, w_down=w_down, final_gain=final_gain)


EPS = 1e-06

def slot_table(route_rows):
    flattened = route_rows.reshape(-1)
    matches = (flattened[:, None] == jnp.arange(EXPERTS, dtype=jnp.int32)[None, :]).astype(jnp.int32)
    earlier = jnp.cumsum(matches, axis=0) - matches
    slot_of = lax.optimization_barrier(jnp.sum(earlier * matches, axis=1))
    return (flattened * CAP + slot_of).reshape(route_rows.shape).astype(jnp.int32)

def dispatch(place_block, row_block):
    slot_ids = jnp.arange(EXPERTS * CAP, dtype=jnp.int32)
    selector = lax.optimization_barrier(jnp.sum((place_block[None, :, :] == slot_ids[:, None, None]).astype(jnp.float32), axis=2))
    return jnp.dot(selector.astype(jnp.bfloat16), row_block, preferred_element_type=jnp.float32).astype(jnp.bfloat16)

def expert(inputs):
    row_block, gate_w, up_w, down_w = inputs
    gate_value = jnp.dot(row_block, gate_w, preferred_element_type=jnp.float32)
    up_value = jnp.dot(row_block, up_w, preferred_element_type=jnp.float32)
    hidden = (jax.nn.silu(gate_value) * up_value).astype(jnp.bfloat16)
    hidden_split = hidden.reshape(row_block.shape[0], N_TP, FF // N_TP).astype(jnp.float32)
    down_split = down_w.reshape(N_TP, FF // N_TP, D).astype(jnp.float32)
    partial_value = jnp.einsum('rjf,jfd->jrd', hidden_split, down_split).astype(jnp.bfloat16)
    partial_value = lax.optimization_barrier(partial_value)
    return lax.optimization_barrier(jnp.sum(partial_value.astype(jnp.float32), axis=0)).astype(jnp.bfloat16)

def reference(tokens, norm_gain, routes, route_weights, w_gate, w_up, w_down, final_gain):
    tokens_f = tokens.astype(jnp.float32)
    inverse = lax.rsqrt(lax.optimization_barrier(jnp.mean(tokens_f * tokens_f, axis=1, keepdims=True)) + EPS)
    normed = (tokens_f * inverse * norm_gain[None, :]).astype(jnp.bfloat16)
    blocks = normed.reshape(N_EP, TOK_DEV, D)
    places = jax.vmap(slot_table)(routes.reshape(N_EP, TOK_DEV, TOP_K))
    buffers = jax.vmap(dispatch)(places, blocks)
    expert_in = buffers.reshape(N_EP, EXPERTS, CAP, D).transpose(1, 0, 2, 3).reshape(EXPERTS, N_EP * CAP, D)
    expert_out = lax.map(expert, (expert_in, w_gate, w_up, w_down))
    by_block = expert_out.reshape(EXPERTS, N_EP, CAP, D).transpose(1, 0, 2, 3).reshape(N_EP, EXPERTS * CAP, D)
    block_ids = jnp.arange(N_EP, dtype=jnp.int32)[:, None, None]
    picked = by_block[block_ids, places].astype(jnp.float32)
    weights = route_weights.reshape(N_EP, TOK_DEV, TOP_K)
    combined = lax.optimization_barrier(jnp.sum(weights[:, :, :, None] * picked, axis=2)).reshape(TOKENS, D)
    inverse_out = lax.rsqrt(lax.optimization_barrier(jnp.mean(combined * combined, axis=1, keepdims=True)) + EPS)
    return (combined * inverse_out * final_gain[None, :]).astype(jnp.bfloat16)
```

```python
import functools

import jax
import jax.numpy as jnp
from jax import lax
from jax.experimental import pallas as pl
from jax.experimental.pallas import tpu as pltpu
from jax.sharding import PartitionSpec as P

TOP_K = 6


EPS = 1e-06
MESH = pl.DeviceIdType.MESH


def slot_table(route_rows, experts_all, capacity):
    flattened = route_rows.reshape(-1)
    matches = (flattened[:, None] == jnp.arange(experts_all, dtype=jnp.int32)[None, :]).astype(
        jnp.int32
    )
    earlier = jnp.cumsum(matches, axis=0) - matches
    slot_of = jnp.sum(earlier * matches, axis=1)
    return (flattened * capacity + slot_of).reshape(route_rows.shape)


def per_device(tokens, norm_gain, routes, route_weights, w_gate, w_up, w_down, final_gain):
    tok_count, features = tokens.shape
    ep_size = lax.axis_size("ep")
    exp_local = w_gate.shape[0]
    experts_all = exp_local * ep_size
    capacity = max(2, min(tok_count, 2 * tok_count * TOP_K // experts_all))
    slot_count = experts_all * capacity
    tokens_f = tokens.astype(jnp.float32)
    inverse = lax.rsqrt(jnp.mean(tokens_f * tokens_f, axis=1, keepdims=True) + EPS)
    normed = (tokens_f * inverse * norm_gain[None, :]).astype(jnp.bfloat16)
    places = slot_table(routes, experts_all, capacity)
    slot_ids = jnp.arange(slot_count, dtype=jnp.int32)
    matched = places[:, :, None] == slot_ids[None, None, :]
    selector = jnp.sum(matched.astype(jnp.float32), axis=1).T.astype(jnp.bfloat16)
    combine_rows = jnp.sum(jnp.where(matched, route_weights[:, :, None], 0.0), axis=1)
    outgoing = jnp.dot(selector, normed, preferred_element_type=jnp.float32).astype(jnp.bfloat16)
    outgoing = outgoing.reshape(ep_size, exp_local, capacity, features)
    received = lax.all_to_all(outgoing, "ep", split_axis=0, concat_axis=0, tiled=True)
    gate_value = jnp.einsum("secd,edf->secf", received, w_gate, preferred_element_type=jnp.float32)
    up_value = jnp.einsum("secd,edf->secf", received, w_up, preferred_element_type=jnp.float32)
    hidden = (jax.nn.silu(gate_value) * up_value).astype(jnp.bfloat16)
    partial_value = jnp.einsum("secf,efd->secd", hidden, w_down, preferred_element_type=jnp.float32)
    summed = lax.psum_scatter(
        partial_value.astype(jnp.bfloat16), "tp", scatter_dimension=3, tiled=True
    )
    returned = lax.all_to_all(summed, "ep", split_axis=0, concat_axis=0, tiled=True)
    results = returned.reshape(slot_count, returned.shape[3]).astype(jnp.float32)
    combined = jnp.dot(combine_rows, results, precision=lax.Precision.HIGHEST)
    local_squares = jnp.sum(combined * combined, axis=1)
    squares_all = lax.psum(local_squares, "tp")
    inverse_out = lax.rsqrt(squares_all / features + EPS)
    return (combined * inverse_out[:, None] * final_gain[None, :]).astype(jnp.bfloat16)


def fused_kernel(nz, tile, tokens_ref, gain_ref, routes_ref, rw_ref, wg_hbm, wu_hbm, wd_hbm, fgain_ref,
                 out_ref, buf, wg, wu, wd, hid, part, dbuf, xbuf, zbuf, wsem,
                 az_s, az_r, ax_s, ax_r, ad_s, ad_r, rd_s, rd_r, rx_s, rx_r, rz_s, rz_r):
    rows, features = tokens_ref.shape
    hidden_units = wg.shape[1]
    experts = 4 * nz
    chunk = 4 * rows
    f32, bf16 = jnp.float32, jnp.bfloat16
    me = lax.axis_index("ep")
    core = lax.rem(me, 2)
    x = lax.rem(lax.div(me, 2), 2)
    z = lax.div(me, 4)
    d_peer = me + 1 - 2 * core
    x_peer = me + 2 - 4 * x

    def z_of(dz):
        return lax.rem(z + dz, nz)

    def z_peer(dz):
        return z_of(dz) * 4 + x * 2 + core

    def weight_copy(which, j):
        src, dst = ((wg_hbm, wg), (wu_hbm, wu), (wd_hbm, wd))[which]
        cols = pl.ds(pl.multiple_of(j * tile, tile), tile)
        return pltpu.make_async_copy(src.at[0, :, cols], dst.at[:, cols], wsem.at[which, j])

    gu_tiles, d_tiles = hidden_units // tile, features // tile
    for j in range(gu_tiles):
        weight_copy(0, j).start()
        weight_copy(1, j).start()
    for j in range(d_tiles):
        weight_copy(2, j).start()

    barrier = pltpu.get_barrier_semaphore()
    peers = [d_peer, x_peer] + [z_peer(dz) for dz in range(1, nz)]
    for peer in peers:
        pl.semaphore_signal(barrier, inc=1, device_id={"ep": peer}, device_id_type=MESH)

    own = pl.ds(pl.multiple_of(me * rows, rows), rows)
    tok = tokens_ref[...].astype(f32)
    inverse = lax.rsqrt(jnp.mean(tok * tok, axis=1, keepdims=True) + EPS)
    buf[own, :features] = (tok * inverse * gain_ref[...]).astype(bf16)
    extra = buf.shape[1] - features
    lanes = lax.broadcasted_iota(jnp.int32, (rows, extra), 1)
    first = jnp.zeros((rows, extra), f32)
    second = jnp.zeros((rows, extra), f32)
    for k in range(routes_ref.shape[1]):
        r, w = routes_ref[:, k:k + 1], rw_ref[:, k:k + 1]
        first = first + jnp.where(lanes == r, w, 0.0)
        second = second + jnp.where(lanes == r + experts, w, 0.0)
    rest = second - second.astype(bf16).astype(f32)
    buf[own, features:] = (first + rest).astype(bf16)

    pl.semaphore_wait(barrier, len(peers))

    def remote(src, dst, s, r, dev):
        return pltpu.make_async_remote_copy(
            src_ref=src, dst_ref=dst, send_sem=s, recv_sem=r, device_id={"ep": dev}, device_id_type=MESH
        )

    def block(e):
        return buf.at[pl.ds(pl.multiple_of(e * rows, rows), rows), :]

    def same_col(dz):
        return block(z_of(nz - dz) * 4 + x * 2 + core)

    def other_col(dz):
        return block(z_of(nz - dz) * 4 + (1 - x) * 2 + core)

    def ag_z(dz, arriving=False):
        ref = same_col(dz) if arriving else block(me)
        return remote(ref, ref, az_s.at[dz], az_r.at[dz], z_peer(dz))

    def ag_x(dz, arriving=False):
        ref = other_col(dz) if arriving else same_col(dz)
        return remote(ref, ref, ax_s.at[dz], ax_r.at[dz], x_peer)

    def ag_d(dz, j, arriving=False):
        if arriving:
            col = x if j == 0 else 1 - x
            ref = block(z_of(nz - dz) * 4 + col * 2 + 1 - core)
        else:
            ref = same_col(dz) if j == 0 else other_col(dz)
        return remote(ref, ref, ad_s.at[dz, j], ad_r.at[dz, j], d_peer)

    def rs_block(dz, same_x, same_core):
        col = x if same_x else 1 - x
        lane = core if same_core else 1 - core
        at = pl.multiple_of((col * 2 + lane) * rows, rows)
        return part.at[dz, pl.ds(at, rows), :]

    def rs_d(dz, j):
        return remote(rs_block(dz, j == 0, False), dbuf.at[dz, j], rd_s.at[dz, j], rd_r.at[dz, j], d_peer)

    def rs_x(dz):
        return remote(rs_block(dz, False, True), xbuf.at[dz], rx_s.at[dz], rx_r.at[dz], x_peer)

    def rs_z(dz):
        return remote(rs_block(dz, True, True), zbuf.at[dz], rz_s.at[dz], rz_r.at[dz], z_peer(nz - dz))

    away = [1] + ([nz - 1] if nz > 2 else []) + list(range(2, nz - 1))
    order = away + [0]

    ag_x(0).start()
    for dz in away:
        ag_z(dz).start()
    ag_d(0, 0).start()

    def forward_z(dz):
        ag_z(dz, True).wait_recv()
        ag_x(dz).start()
        ag_d(dz, 0).start()

    def forward_x(dz):
        ag_x(dz, True).wait_recv()
        ag_d(dz, 1).start()

    def chunk_rows(dz):
        return pl.ds(pl.multiple_of(z_of(nz - dz) * chunk, chunk), chunk)

    def gate_up(dz, begin, end, wait):
        here = chunk_rows(dz)

        def body(j, carry):
            if wait:
                weight_copy(0, j).wait()
                weight_copy(1, j).wait()
            cols = pl.ds(pl.multiple_of(j * tile, tile), tile)
            lhs = buf[here, :features]
            g = jnp.dot(lhs, wg[:, cols], preferred_element_type=f32)
            u = jnp.dot(lhs, wu[:, cols], preferred_element_type=f32)
            hid[:, cols] = (g / (1.0 + jnp.exp(-g)) * u).astype(bf16)
            return carry

        lax.fori_loop(begin, end, body, 0)

    def down(dz, wait):
        ext = buf[chunk_rows(dz), features:].astype(f32)
        lane = lax.broadcasted_iota(jnp.int32, ext.shape, 1)
        mine = jnp.logical_or(lane == me, lane == me + experts)
        weight = jnp.sum(jnp.where(mine, ext, 0.0), axis=1, keepdims=True)

        def body(j, carry):
            if wait:
                weight_copy(2, j).wait()
            cols = pl.ds(pl.multiple_of(j * tile, tile), tile)
            o = jnp.dot(hid[...], wd[:, cols], preferred_element_type=f32)
            part[dz, :, cols] = (o * weight).astype(bf16)
            return carry

        lax.fori_loop(0, d_tiles, body, 0)

    def finish_d(dz):
        rs_d(dz, 1).wait_recv()
        ref = rs_block(dz, False, True)
        ref[...] = (ref[...].astype(f32) + dbuf[dz, 1].astype(f32)).astype(bf16)
        rs_d(dz, 0).wait_recv()
        rs_x(dz).start()

    def finish_x(dz):
        rs_x(dz).wait_recv()
        ref = rs_block(dz, True, True)
        total = ref[...].astype(f32) + dbuf[dz, 0].astype(f32) + xbuf[dz].astype(f32)
        if dz == 0:
            return total
        ref[...] = total.astype(bf16)
        return None

    for dz in away:
        forward_z(dz)
    forward_x(0)
    forward_x(order[0])

    half = max(1, gu_tiles // 2)
    for i, dz in enumerate(order):
        if dz == 0:
            ag_d(0, 0, True).wait_recv()
            ag_d(0, 1, True).wait_recv()
        else:
            ag_d(dz, 0, True).wait_recv()
            ag_d(dz, 1, True).wait_recv()
        gate_up(dz, 0, half, i == 0)
        if i >= 1:
            finish_d(order[i - 1])
        gate_up(dz, half, gu_tiles, i == 0)
        if i + 1 < len(order) and order[i + 1] != 0:
            forward_x(order[i + 1])
        if i >= 2:
            finish_x(order[i - 2])
        down(dz, i == 0)
        if i >= 2:
            rs_z(order[i - 2]).start()
        rs_d(dz, 1).start()
        rs_d(dz, 0).start()

    if len(order) >= 2:
        finish_x(order[-2])
    finish_d(0)
    if len(order) >= 2:
        rs_z(order[-2]).start()
    total = finish_x(0)
    for dz in away:
        rs_z(dz).wait_recv()
        total = total + zbuf[dz].astype(f32)
    inverse_out = lax.rsqrt(jnp.mean(total * total, axis=1, keepdims=True) + EPS)
    out_ref[...] = (total * inverse_out * fgain_ref[...]).astype(out_ref.dtype)

    for dz in order:
        ag_x(dz).wait_send()
        rs_x(dz).wait_send()
        for j in range(2):
            ag_d(dz, j).wait_send()
            rs_d(dz, j).wait_send()
        if dz:
            ag_z(dz).wait_send()
            rs_z(dz).wait_send()


def fused_device(tokens, norm_gain, routes, route_weights, w_gate, w_up, w_down, final_gain):
    rows, features = tokens.shape
    hidden_units = w_gate.shape[2]
    experts = lax.axis_size("ep")
    nz = experts // 4
    tile = 512
    extra = -(-2 * experts // 128) * 128
    vmem, anywhere = pl.BlockSpec(memory_space=pltpu.VMEM), pl.BlockSpec(memory_space=pl.ANY)
    dma = pltpu.SemaphoreType.DMA
    bf16 = jnp.bfloat16
    tiles = max(hidden_units, features) // tile
    return pl.pallas_call(
        functools.partial(fused_kernel, nz, tile),
        out_shape=jax.ShapeDtypeStruct((rows, features), jnp.bfloat16),
        in_specs=[vmem, vmem, vmem, vmem, anywhere, anywhere, anywhere, vmem],
        out_specs=vmem,
        scratch_shapes=[
            pltpu.VMEM((experts * rows, features + extra), bf16),
            pltpu.VMEM((features, hidden_units), bf16),
            pltpu.VMEM((features, hidden_units), bf16),
            pltpu.VMEM((hidden_units, features), bf16),
            pltpu.VMEM((4 * rows, hidden_units), bf16),
            pltpu.VMEM((nz, 4 * rows, features), bf16),
            pltpu.VMEM((nz, 2, rows, features), bf16),
            pltpu.VMEM((nz, rows, features), bf16),
            pltpu.VMEM((nz, rows, features), bf16),
            dma((3, tiles)),
            dma((nz,)), dma((nz,)), dma((nz,)), dma((nz,)), dma((nz, 2)), dma((nz, 2)),
            dma((nz, 2)), dma((nz, 2)), dma((nz,)), dma((nz,)), dma((nz,)), dma((nz,)),
        ],
        compiler_params=pltpu.CompilerParams(
            collective_id=0, has_side_effects=True, vmem_limit_bytes=60 * 1024 * 1024
        ),
    )(tokens, norm_gain[None, :], routes, route_weights, w_gate, w_up, w_down, final_gain[None, :])


def solution(mesh):
    placed = (
        P(("grp", "ep"), None),
        P(),
        P(("grp", "ep"), None),
        P(("grp", "ep"), None),
        P("ep", None, "tp"),
        P("ep", None, "tp"),
        P("ep", "tp", None),
        P("tp"),
    )
    ep, tp = mesh.shape["ep"], mesh.shape["tp"]

    def step(*args):
        rows, features = args[0].shape
        hidden_units = args[4].shape[2]
        fits = 3 * features * hidden_units + 3 * ep * rows * features < 24 * 2 ** 20
        whole_tiles = features % 512 == 0 and hidden_units % 512 == 0 and rows % 16 == 0
        if tp == 1 and ep % 4 == 0 and ep > 4 and args[4].shape[0] == 1 and fits and whole_tiles:
            return fused_device(*args)
        return per_device(*args)

    return jax.shard_map(
        step, mesh=mesh, in_specs=placed, out_specs=P(("grp", "ep"), "tp"), check_vma=False
    )
```

```python
import functools

import jax
import jax.numpy as jnp
from jax import lax
from jax.experimental import pallas as pl
from jax.experimental.pallas import tpu as pltpu
from jax.sharding import PartitionSpec as P

TOP_K = 6


EPS = 1e-06
MESH = pl.DeviceIdType.MESH


def slot_table(route_rows, experts_all, capacity):
    flattened = route_rows.reshape(-1)
    matches = (flattened[:, None] == jnp.arange(experts_all, dtype=jnp.int32)[None, :]).astype(
        jnp.int32
    )
    earlier = jnp.cumsum(matches, axis=0) - matches
    slot_of = jnp.sum(earlier * matches, axis=1)
    return (flattened * capacity + slot_of).reshape(route_rows.shape)


def per_device(tokens, norm_gain, routes, route_weights, w_gate, w_up, w_down, final_gain):
    tok_count, features = tokens.shape
    ep_size = lax.axis_size("ep")
    exp_local = w_gate.shape[0]
    experts_all = exp_local * ep_size
    capacity = max(2, min(tok_count, 2 * tok_count * TOP_K // experts_all))
    slot_count = experts_all * capacity
    tokens_f = tokens.astype(jnp.float32)
    inverse = lax.rsqrt(jnp.mean(tokens_f * tokens_f, axis=1, keepdims=True) + EPS)
    normed = (tokens_f * inverse * norm_gain[None, :]).astype(jnp.bfloat16)
    places = slot_table(routes, experts_all, capacity)
    slot_ids = jnp.arange(slot_count, dtype=jnp.int32)
    matched = places[:, :, None] == slot_ids[None, None, :]
    selector = jnp.sum(matched.astype(jnp.float32), axis=1).T.astype(jnp.bfloat16)
    combine_rows = jnp.sum(jnp.where(matched, route_weights[:, :, None], 0.0), axis=1)
    outgoing = jnp.dot(selector, normed, preferred_element_type=jnp.float32).astype(jnp.bfloat16)
    outgoing = outgoing.reshape(ep_size, exp_local, capacity, features)
    received = lax.all_to_all(outgoing, "ep", split_axis=0, concat_axis=0, tiled=True)
    gate_value = jnp.einsum("secd,edf->secf", received, w_gate, preferred_element_type=jnp.float32)
    up_value = jnp.einsum("secd,edf->secf", received, w_up, preferred_element_type=jnp.float32)
    hidden = (jax.nn.silu(gate_value) * up_value).astype(jnp.bfloat16)
    partial_value = jnp.einsum("secf,efd->secd", hidden, w_down, preferred_element_type=jnp.float32)
    summed = lax.psum_scatter(
        partial_value.astype(jnp.bfloat16), "tp", scatter_dimension=3, tiled=True
    )
    returned = lax.all_to_all(summed, "ep", split_axis=0, concat_axis=0, tiled=True)
    results = returned.reshape(slot_count, returned.shape[3]).astype(jnp.float32)
    combined = jnp.dot(combine_rows, results, precision=lax.Precision.HIGHEST)
    local_squares = jnp.sum(combined * combined, axis=1)
    squares_all = lax.psum(local_squares, "tp")
    inverse_out = lax.rsqrt(squares_all / features + EPS)
    return (combined * inverse_out[:, None] * final_gain[None, :]).astype(jnp.bfloat16)


def fused_kernel(nz, tile, tokens_ref, gain_ref, routes_ref, rw_ref, wg_hbm, wu_hbm, wd_hbm, fgain_ref,
                 out_ref, buf, wg, wu, wd, hid, part, dbuf, xbuf, zbuf, wsem,
                 az_s, az_r, ax_s, ax_r, ad_s, ad_r, rd_s, rd_r, rx_s, rx_r, rz_s, rz_r):
    rows, features = tokens_ref.shape
    hidden_units = wg.shape[1]
    experts = 4 * nz
    chunk = 4 * rows
    f32, bf16 = jnp.float32, jnp.bfloat16
    me = lax.axis_index("ep")
    core = lax.rem(me, 2)
    x = lax.rem(lax.div(me, 2), 2)
    z = lax.div(me, 4)
    d_peer = me + 1 - 2 * core
    x_peer = me + 2 - 4 * x

    def z_of(dz):
        return lax.rem(z + dz, nz)

    def z_peer(dz):
        return z_of(dz) * 4 + x * 2 + core

    def weight_copy(which, j):
        src, dst = ((wg_hbm, wg), (wu_hbm, wu), (wd_hbm, wd))[which]
        cols = pl.ds(pl.multiple_of(j * tile, tile), tile)
        return pltpu.make_async_copy(src.at[0, :, cols], dst.at[:, cols], wsem.at[which, j])

    gu_tiles, d_tiles = hidden_units // tile, features // tile
    for j in range(gu_tiles):
        weight_copy(0, j).start()
        weight_copy(1, j).start()
    for j in range(d_tiles):
        weight_copy(2, j).start()

    barrier = pltpu.get_barrier_semaphore()
    peers = [d_peer, x_peer] + [z_peer(dz) for dz in range(1, nz)]
    for peer in peers:
        pl.semaphore_signal(barrier, inc=1, device_id={"ep": peer}, device_id_type=MESH)

    own = pl.ds(pl.multiple_of(me * rows, rows), rows)
    tok = tokens_ref[...].astype(f32)
    inverse = lax.rsqrt(jnp.mean(tok * tok, axis=1, keepdims=True) + EPS)
    buf[own, :features] = (tok * inverse * gain_ref[...]).astype(bf16)
    extra = buf.shape[1] - features
    lanes = lax.broadcasted_iota(jnp.int32, (rows, extra), 1)
    first = jnp.zeros((rows, extra), f32)
    second = jnp.zeros((rows, extra), f32)
    for k in range(routes_ref.shape[1]):
        r, w = routes_ref[:, k:k + 1], rw_ref[:, k:k + 1]
        first = first + jnp.where(lanes == r, w, 0.0)
        second = second + jnp.where(lanes == r + experts, w, 0.0)
    rest = second - second.astype(bf16).astype(f32)
    buf[own, features:] = (first + rest).astype(bf16)

    pl.semaphore_wait(barrier, len(peers))

    def remote(src, dst, s, r, dev):
        return pltpu.make_async_remote_copy(
            src_ref=src, dst_ref=dst, send_sem=s, recv_sem=r, device_id={"ep": dev}, device_id_type=MESH
        )

    def block(e):
        return buf.at[pl.ds(pl.multiple_of(e * rows, rows), rows), :]

    own_step = nz - 1
    tables = [sorted((p for p in range(nz) if p != q), key=lambda p: (abs(p - q), p)) for q in range(nz)]
    places = []
    for i in range(own_step):
        value = tables[0][i]
        for q in range(1, nz):
            value = jnp.where(z == q, tables[q][i], value)
        places.append(value)
    places.append(z)

    def same_col(i):
        return block(places[i] * 4 + x * 2 + core)

    def other_col(i):
        return block(places[i] * 4 + (1 - x) * 2 + core)

    def ag_z(i, up):
        ref = same_col(i)
        peer = me + 4 if up else me - 4
        return remote(ref, ref, az_s.at[i, int(up)], az_r.at[places[i]], peer)

    def ag_x(i, arriving=False):
        ref = other_col(i) if arriving else same_col(i)
        return remote(ref, ref, ax_s.at[i], ax_r.at[i], x_peer)

    def ag_d(i, j, arriving=False):
        if arriving:
            col = x if j == 0 else 1 - x
            ref = block(places[i] * 4 + col * 2 + 1 - core)
        else:
            ref = same_col(i) if j == 0 else other_col(i)
        return remote(ref, ref, ad_s.at[i, j], ad_r.at[i, j], d_peer)

    def rs_block(i, same_x, same_core):
        col = x if same_x else 1 - x
        lane = core if same_core else 1 - core
        at = pl.multiple_of((col * 2 + lane) * rows, rows)
        return part.at[i, pl.ds(at, rows), :]

    def rs_d(i, j):
        return remote(rs_block(i, j == 0, False), dbuf.at[i, j], rd_s.at[i, j], rd_r.at[i, j], d_peer)

    def rs_x(i):
        return remote(rs_block(i, False, True), xbuf.at[i], rx_s.at[i], rx_r.at[i], x_peer)

    def rs_z(i):
        peer = places[i] * 4 + x * 2 + core
        return remote(rs_block(i, True, True), zbuf.at[z], rz_s.at[i], rz_r.at[z], peer)

    def rs_z_arriving(i):
        peer = places[i] * 4 + x * 2 + core
        ref = zbuf.at[places[i]]
        return remote(ref, ref, rz_s.at[i], rz_r.at[places[i]], peer)

    def pass_on(i, action):
        from_below, from_above = places[i] <= z, places[i] >= z

        @pl.when(jnp.logical_and(from_below, z < nz - 1))
        def _():
            action(ag_z(i, True))

        @pl.when(jnp.logical_and(from_above, z > 0))
        def _():
            action(ag_z(i, False))

    pass_on(own_step, lambda copy: copy.start())
    ag_x(own_step).start()
    ag_d(own_step, 0).start()

    def forward_z(i):
        ag_z(i, True).wait_recv()
        pass_on(i, lambda copy: copy.start())
        ag_x(i).start()
        ag_d(i, 0).start()

    def forward_x(i):
        ag_x(i, True).wait_recv()
        ag_d(i, 1).start()

    def chunk_rows(i):
        return pl.ds(pl.multiple_of(places[i] * chunk, chunk), chunk)

    def gate_up(i, begin, end, wait):
        here = chunk_rows(i)

        def body(j, carry):
            if wait:
                weight_copy(0, j).wait()
                weight_copy(1, j).wait()
            cols = pl.ds(pl.multiple_of(j * tile, tile), tile)
            lhs = buf[here, :features]
            g = jnp.dot(lhs, wg[:, cols], preferred_element_type=f32)
            u = jnp.dot(lhs, wu[:, cols], preferred_element_type=f32)
            hid[:, cols] = (g / (1.0 + jnp.exp(-g)) * u).astype(bf16)
            return carry

        lax.fori_loop(begin, end, body, 0)

    def down(i, begin, end, wait):
        ext = buf[chunk_rows(i), features:].astype(f32)
        lane = lax.broadcasted_iota(jnp.int32, ext.shape, 1)
        mine = jnp.logical_or(lane == me, lane == me + experts)
        weight = jnp.sum(jnp.where(mine, ext, 0.0), axis=1, keepdims=True)

        def body(j, carry):
            if wait:
                weight_copy(2, j).wait()
            cols = pl.ds(pl.multiple_of(j * tile, tile), tile)
            o = jnp.dot(hid[...], wd[:, cols], preferred_element_type=f32)
            part[i, :, cols] = (o * weight).astype(bf16)
            return carry

        lax.fori_loop(begin, end, body, 0)

    def finish_d(i):
        rs_d(i, 1).wait_recv()
        ref = rs_block(i, False, True)
        ref[...] = (ref[...].astype(f32) + dbuf[i, 1].astype(f32)).astype(bf16)
        rs_d(i, 0).wait_recv()
        rs_x(i).start()

    def finish_x(i):
        rs_x(i).wait_recv()
        ref = rs_block(i, True, True)
        total = ref[...].astype(f32) + dbuf[i, 0].astype(f32) + xbuf[i].astype(f32)
        if i == own_step:
            return total
        ref[...] = total.astype(bf16)
        rs_z(i).start()
        return None

    forward_z(0)
    forward_x(own_step)
    forward_z(1)
    forward_x(0)

    gu_half, d_half = max(1, gu_tiles // 2), max(1, d_tiles // 2)
    for i in range(nz):
        ag_d(i, 0, True).wait_recv()
        ag_d(i, 1, True).wait_recv()
        gate_up(i, 0, gu_half, i == 0)
        if i >= 1:
            finish_d(i - 1)
        gate_up(i, gu_half, gu_tiles, i == 0)
        down(i, 0, d_half, i == 0)
        if i + 1 < own_step:
            forward_x(i + 1)
        if i >= 2:
            finish_x(i - 2)
        down(i, d_half, d_tiles, i == 0)
        rs_d(i, 1).start()
        rs_d(i, 0).start()
        if i + 2 < own_step:
            forward_z(i + 2)

    finish_d(own_step)
    finish_x(own_step - 1)
    total = finish_x(own_step)
    for i in range(own_step):
        rs_z_arriving(i).wait_recv()
        total = total + zbuf[places[i]].astype(f32)
    inverse_out = lax.rsqrt(jnp.mean(total * total, axis=1, keepdims=True) + EPS)
    out_ref[...] = (total * inverse_out * fgain_ref[...]).astype(out_ref.dtype)

    for i in range(nz):
        pass_on(i, lambda copy: copy.wait_send())
        ag_x(i).wait_send()
        rs_x(i).wait_send()
        for j in range(2):
            ag_d(i, j).wait_send()
            rs_d(i, j).wait_send()
        if i < own_step:
            rs_z(i).wait_send()


def fused_device(tokens, norm_gain, routes, route_weights, w_gate, w_up, w_down, final_gain):
    rows, features = tokens.shape
    hidden_units = w_gate.shape[2]
    experts = lax.axis_size("ep")
    nz = experts // 4
    tile = 1024
    extra = -(-2 * experts // 128) * 128
    vmem, anywhere = pl.BlockSpec(memory_space=pltpu.VMEM), pl.BlockSpec(memory_space=pl.ANY)
    dma = pltpu.SemaphoreType.DMA
    bf16 = jnp.bfloat16
    tiles = max(hidden_units, features) // tile
    return pl.pallas_call(
        functools.partial(fused_kernel, nz, tile),
        out_shape=jax.ShapeDtypeStruct((rows, features), jnp.bfloat16),
        in_specs=[vmem, vmem, vmem, vmem, anywhere, anywhere, anywhere, vmem],
        out_specs=vmem,
        scratch_shapes=[
            pltpu.VMEM((experts * rows, features + extra), bf16),
            pltpu.VMEM((features, hidden_units), bf16),
            pltpu.VMEM((features, hidden_units), bf16),
            pltpu.VMEM((hidden_units, features), bf16),
            pltpu.VMEM((4 * rows, hidden_units), bf16),
            pltpu.VMEM((nz, 4 * rows, features), bf16),
            pltpu.VMEM((nz, 2, rows, features), bf16),
            pltpu.VMEM((nz, rows, features), bf16),
            pltpu.VMEM((nz, rows, features), bf16),
            dma((3, tiles)),
            dma((nz, 2)), dma((nz,)), dma((nz,)), dma((nz,)), dma((nz, 2)), dma((nz, 2)),
            dma((nz, 2)), dma((nz, 2)), dma((nz,)), dma((nz,)), dma((nz,)), dma((nz,)),
        ],
        compiler_params=pltpu.CompilerParams(
            collective_id=0, has_side_effects=True, vmem_limit_bytes=60 * 1024 * 1024
        ),
    )(tokens, norm_gain[None, :], routes, route_weights, w_gate, w_up, w_down, final_gain[None, :])


def solution(mesh):
    placed = (
        P(("grp", "ep"), None),
        P(),
        P(("grp", "ep"), None),
        P(("grp", "ep"), None),
        P("ep", None, "tp"),
        P("ep", None, "tp"),
        P("ep", "tp", None),
        P("tp"),
    )
    ep, tp = mesh.shape["ep"], mesh.shape["tp"]

    def step(*args):
        rows, features = args[0].shape
        hidden_units = args[4].shape[2]
        fits = 3 * features * hidden_units + 3 * ep * rows * features < 24 * 2 ** 20
        whole_tiles = features % 1024 == 0 and hidden_units % 1024 == 0 and rows % 16 == 0
        if tp == 1 and ep % 4 == 0 and ep >= 12 and args[4].shape[0] == 1 and fits and whole_tiles:
            return fused_device(*args)
        return per_device(*args)

    return jax.shard_map(
        step, mesh=mesh, in_specs=placed, out_specs=P(("grp", "ep"), "tp"), check_vma=False
    )
```
